256 devices in a mesh: rep: 2 (over z_hi), fs: 16 (over z_lo, y), tp: 8 (over x, core).
Axes of the slice: x: 4, y: 4, z: 8 (z_hi: 2, z_lo: 4; z = z_hi * 4 + z_lo), core: 2. Of those that a mesh axis runs over, the one named last changes fastest.
Arguments:
- stream: bfloat16 [16384, 2048], P(('rep', 'fs'), 'tp'), may hold values from -6 to 6
- recurrent_norm_gain: float32 [2048], replicated, may hold values from 0.1 to 1.9
- feedforward_norm_gain: float32 [2048], replicated, may hold values from 0.1 to 1.9
- recurrent_input_weight: bfloat16 [2048, 2048], P('fs', 'tp'), may hold values from -0.125 to 0.125
- output_gate_weight: bfloat16 [2048, 2048], P('fs', 'tp'), may hold values from -0.125 to 0.125
- causal_filter_weight: bfloat16 [4, 2048], P(None, 'tp'), may hold values from -3 to 3
- decay_gate_matrix: bfloat16 [32, 64, 64], P('tp'), may hold values from -0.75 to 0.75
- input_gate_matrix: bfloat16 [32, 64, 64], P('tp'), may hold values from -0.75 to 0.75
- channel_decay_param: float32 [2048], P('tp'), may hold values from 3 to 10
- token_decay_offset: float32 [16384, 2048], P(('rep', 'fs'), 'tp'), may hold values from -0.7 to 0, as said below
- recurrent_output_weight: bfloat16 [2048, 2048], P('tp', 'fs'), may hold values from -0.125 to 0.125
- up_projection_weight: bfloat16 [2048, 6144], P('fs', 'tp'), may hold values from -0.125 to 0.125
- down_projection_weight: bfloat16 [6144, 2048], P('tp', 'fs'), may hold values from -0.078125 to 0.078125
Outputs:
- updated: bfloat16 [16384, 2048], P(('rep', 'fs'), 'tp')
The draws below stay inside these ranges and needn't reach their ends.
Inputs may be any that keep to these rules, and one draw needn't show every extreme that they name: `token_decay_offset`: zero except at a few positions, where a whole row is negative.
All inputs are finite; a program needn't handle non-finite values.
Results may differ from the reference program's by a relative error of at most 0.015.
Values may be sent and summed in bfloat16 or wider, within the bound.
No kernel may reach another device: no remote copies, remote signals or barrier semaphores. Data moves between devices by JAX's collectives and lax.ppermute only.
A program may use at most 64 MiB of HBM per device.

```python
import jax
import jax.numpy as jnp
from jax import lax

D = 2048
FF = 6144
BLOCK = 64
CONV = 4
SEQ_LEN = 128
TOKENS = 16384
BLOCKS = 32
N_TP = 8


def draw_channel_decay_param(key, part):
    kind_key = jax.random.fold_in(key, 11)
    slow_key = jax.random.fold_in(key, 12)
    fast_key = jax.random.fold_in(key, 13)
    fast = jax.random.uniform(kind_key, (D,), jnp.float32) < 0.5
    slow_rate = jnp.exp(jax.random.uniform(slow_key, (D,), jnp.float32, jnp.log(0.3), jnp.log(3.0))) / SEQ_LEN
    fast_rate = jnp.exp(jax.random.uniform(fast_key, (D,), jnp.float32, jnp.log(0.1), jnp.log(0.3)))
    rate = jnp.where(fast, fast_rate, slow_rate)
    return (-jnp.log(jnp.expm1(rate / 8.0))).astype(jnp.float32)


def draw_token_decay_offset(key, part):
    where_key = jax.random.fold_in(key, 21)
    depth_key = jax.random.fold_in(key, 22)
    hits = jax.random.uniform(where_key, (TOKENS, 1), jnp.float32) < 3.0 / SEQ_LEN
    depth = jax.random.uniform(depth_key, (TOKENS, D), jnp.float32, 0.22, 0.69)
    return jnp.where(hits, -depth, 0.0).astype(jnp.float32)


def block_scale(own_key, shape, cuts, least, high):
    loudness = 1.0
    for position, blocks in cuts:
        heights = jax.random.uniform(jax.random.fold_in(jax.random.fold_in(own_key, 6), position), (blocks,), jnp.float32, least / len(cuts), high / len(cuts))
        loudness = loudness * jnp.repeat(jnp.exp(heights), shape[position] // blocks).reshape((-1,) + (1,) * (len(shape) - 1 - position))
    return loudness


def noise(rng, shape, width, most, shards=(), kind=jnp.bfloat16):
    array = width * jax.random.normal(rng, shape, jnp.float32)
    if shards:
        array = array * block_scale(rng, shape, shards, -0.22, 0.18)
    return jnp.clip(array, -most, most).astype(kind)


def setup_inputs(seed: int = 0) -> dict:
    seeds = jax.random.split(jax.random.key(seed), 14)
    return {
        "stream": noise(seeds[0], (TOKENS, D), 1.0, 6.0, ((0, 32), (1, 8))),
        "recurrent_norm_gain": jnp.clip(1.0 + 0.18 * jax.random.normal(seeds[1], (D,), jnp.float32), 0.1, 1.9),
        "feedforward_norm_gain": jnp.clip(1.0 + 0.18 * jax.random.normal(seeds[2], (D,), jnp.float32), 0.1, 1.9),
        "recurrent_input_weight": noise(seeds[3], (D, D), D ** -0.5, 0.125, ((0, 16), (1, 8))),
        "output_gate_weight": noise(seeds[4], (D, D), D ** -0.5, 0.125, ((0, 16), (1, 8))),
        "causal_filter_weight": noise(seeds[5], (CONV, D), CONV ** -0.5, 3.0, ((1, 8),)),
        "decay_gate_matrix": noise(seeds[6], (BLOCKS, BLOCK, BLOCK), BLOCK ** -0.5, 0.75, ((0, 8),)),
        "input_gate_matrix": noise(seeds[7], (BLOCKS, BLOCK, BLOCK), BLOCK ** -0.5, 0.75, ((0, 8),)),
        "channel_decay_param": draw_channel_decay_param(jax.random.fold_in(seeds[13], 71), 0),
        "token_decay_offset": draw_token_decay_offset(jax.random.fold_in(seeds[13], 71), 0),
        "recurrent_output_weight": noise(seeds[10], (D, D), D ** -0.5, 0.125, ((0, 8), (1, 16))),
        "up_projection_weight": noise(seeds[11], (D, FF), D ** -0.5, 0.125, ((0, 16), (1, 8))),
        "down_projection_weight": noise(seeds[12], (FF, D), FF ** -0.5, 0.078125, ((0, 8), (1, 16))),
    }


EPSILON = 1e-06
DECAY_MULTIPLIER = 8.0

def norm_rows(values, gain):
    widened = values.astype(jnp.float32)
    inverse = lax.rsqrt(lax.optimization_barrier(jnp.mean(widened * widened, axis=-1, keepdims=True)) + EPSILON)
    return (widened * inverse * gain).astype(jnp.bfloat16)

def short_filter(values, causal_filter_weight):
    positions, channels = values.shape
    sequences = positions // SEQ_LEN
    reach = causal_filter_weight.shape[0]
    widened = lax.optimization_barrier(values).astype(jnp.float32).reshape(sequences, SEQ_LEN, channels)
    padded = jnp.pad(widened, ((0, 0), (reach - 1, 0), (0, 0)))
    taps = causal_filter_weight.astype(jnp.float32)
    total = taps[0] * padded[:, 0:SEQ_LEN]
    for offset in range(1, reach):
        total = total + taps[offset] * padded[:, offset:offset + SEQ_LEN]
    return total.reshape(positions, channels).astype(jnp.bfloat16)

def combine(earlier, later):
    return (earlier[0] * later[0], later[0] * earlier[1] + later[1])

def recurrent_states(filtered_input, output_gate_rows, decay_gate_matrix, input_gate_matrix, channel_decay_param, token_decay_offset):
    positions, channels = filtered_input.shape
    blocks, block_size, _ = decay_gate_matrix.shape
    widened = lax.optimization_barrier(filtered_input).astype(jnp.float32)
    grouped = widened.reshape(positions, blocks, block_size)
    recurrent_step = jax.nn.sigmoid(jnp.einsum('tnc,ncd->tnd', grouped, decay_gate_matrix.astype(jnp.float32)).reshape(positions, channels))
    inputs = jax.nn.sigmoid(jnp.einsum('tnc,ncd->tnd', grouped, input_gate_matrix.astype(jnp.float32)).reshape(positions, channels))
    decay_logarithm = -DECAY_MULTIPLIER * recurrent_step * jax.nn.softplus(-channel_decay_param) + token_decay_offset
    drive = jnp.sqrt(-jnp.expm1(2.0 * decay_logarithm)) * inputs * widened
    shaped = (positions // SEQ_LEN, SEQ_LEN, channels)
    _, states = lax.associative_scan(combine, (jnp.exp(decay_logarithm).reshape(shaped), drive.reshape(shaped)), axis=1)
    gate_wide = lax.optimization_barrier(output_gate_rows).astype(jnp.float32)
    return (states.reshape(positions, channels) * jax.nn.gelu(gate_wide, approximate=False)).astype(jnp.bfloat16)

def reference(stream, recurrent_norm_gain, feedforward_norm_gain, recurrent_input_weight, output_gate_weight, causal_filter_weight, decay_gate_matrix, input_gate_matrix, channel_decay_param, token_decay_offset, recurrent_output_weight, up_projection_weight, down_projection_weight):
    normed = norm_rows(stream, recurrent_norm_gain)
    span = D // N_TP
    grouped_block_rows = span // BLOCK
    mixer_update = jnp.zeros(stream.shape, jnp.float32)
    for channel_group in range(N_TP):
        lower_bound = channel_group * span
        upper_bound = lower_bound + span
        values = jnp.dot(normed, recurrent_input_weight[:, lower_bound:upper_bound], preferred_element_type=jnp.float32).astype(jnp.bfloat16)
        gate_values = jnp.dot(normed, output_gate_weight[:, lower_bound:upper_bound], preferred_element_type=jnp.float32).astype(jnp.bfloat16)
        filtered_input = short_filter(values, causal_filter_weight[:, lower_bound:upper_bound])
        mixed_rows = recurrent_states(filtered_input, gate_values, decay_gate_matrix[channel_group * grouped_block_rows:(channel_group + 1) * grouped_block_rows], input_gate_matrix[channel_group * grouped_block_rows:(channel_group + 1) * grouped_block_rows], channel_decay_param[lower_bound:upper_bound], token_decay_offset[:, lower_bound:upper_bound])
        partial_value = jnp.dot(mixed_rows, recurrent_output_weight[lower_bound:upper_bound], preferred_element_type=jnp.float32).astype(jnp.bfloat16)
        mixer_update = mixer_update + lax.optimization_barrier(partial_value).astype(jnp.float32)
    middle = (stream.astype(jnp.float32) + mixer_update).astype(jnp.bfloat16)
    normed_mid = norm_rows(middle, feedforward_norm_gain)
    hidden_span = FF // N_TP
    channel_update = jnp.zeros(stream.shape, jnp.float32)
    for channel_group in range(N_TP):
        lower_bound = channel_group * hidden_span
        upper_bound = lower_bound + hidden_span
        raised = jnp.dot(normed_mid, up_projection_weight[:, lower_bound:upper_bound], preferred_element_type=jnp.float32)
        activity = jnp.square(jax.nn.relu(raised)).astype(jnp.bfloat16)
        partial_value = jnp.dot(activity, down_projection_weight[lower_bound:upper_bound], preferred_element_type=jnp.float32).astype(jnp.bfloat16)
        channel_update = channel_update + lax.optimization_barrier(partial_value).astype(jnp.float32)
    return (middle.astype(jnp.float32) + channel_update).astype(jnp.bfloat16)
```

```python
import jax
import jax.numpy as jnp
from jax import lax
from jax.experimental import pallas as pl
from jax.experimental.pallas import tpu as pltpu
from jax.sharding import Mesh
from jax.sharding import PartitionSpec as P

SEQ_LEN = 128
EPSILON = 1e-06
DECAY_MULTIPLIER = 8.0
FS = ("zl", "y")
TP = ("x", "c")
REP_FS = ("zh", "zl", "y")
Z = ("zh", "zl")
Z_SIZE = 8
LINE = 4


def shifted(value, axis, offset):
    size = Z_SIZE if axis == Z else LINE
    return lax.ppermute(value, axis, [((i + offset) % size, i) for i in range(size)])


def swapped(value):
    return lax.ppermute(value, "c", [(0, 1), (1, 0)])


def from_ring(value, axis):
    after = shifted(value, axis, 1)
    before = shifted(value, axis, -1)
    across = shifted(value, axis, 2)
    return [value, after, across, before]


def from_group(value):
    own = from_ring(value, "x")
    return [(block, swapped(block)) for block in own]


def vmem_call(body, out_shape, scratch, name, flops=0):
    def run(*args):
        return pl.pallas_call(
            body,
            out_shape=out_shape,
            in_specs=[pl.BlockSpec(memory_space=pltpu.VMEM)] * len(args),
            out_specs=jax.tree.map(lambda _: pl.BlockSpec(memory_space=pltpu.VMEM), out_shape),
            scratch_shapes=scratch,
            name=name,
            compiler_params=pltpu.CompilerParams(vmem_limit_bytes=40 * 1024 * 1024),
            cost_estimate=pl.CostEstimate(flops=flops, bytes_accessed=0, transcendentals=0),
        )(*args)

    return run


def column_of(offset, core):
    x = lax.axis_index("x")
    c = lax.axis_index("c")
    return pl.multiple_of((2 * ((x + offset) % LINE) + (c + core) % 2) * 256, 256)


def piece_of(z_offset, y_offset):
    z = lax.axis_index("zl")
    y = lax.axis_index("y")
    return pl.multiple_of((((z + z_offset) % LINE) * LINE + (y + y_offset) % LINE) * 128, 128)


def norm_into(blocks, gain, rows, normed):
    total = jnp.zeros((SEQ_LEN, 256), jnp.float32)
    for block in blocks:
        wide = block[rows, :].astype(jnp.float32)
        total = total + wide * wide
    mean = jnp.sum(total, axis=-1, keepdims=True) * (1.0 / 2048.0)
    inverse = lax.rsqrt(mean + EPSILON)
    for k, block in enumerate(blocks):
        column = column_of(k // 2, k % 2)
        wide = block[rows, :].astype(jnp.float32)
        scaled = wide * inverse * gain[:, pl.ds(column, 256)]
        normed[rows, pl.ds(column, 256)] = scaled.astype(jnp.bfloat16)


def earlier(value, steps, fill):
    if steps % 8 == 0:
        head = jnp.full((steps, value.shape[1]), fill, value.dtype)
        return jnp.concatenate([head, value[: value.shape[0] - steps]], axis=0)
    moved = pltpu.roll(value, shift=steps, axis=0)
    position = lax.broadcasted_iota(jnp.int32, value.shape, 0)
    return jnp.where(position >= steps, moved, fill)


def recurrence_body(*refs):
    blocks = refs[0:8]
    pieces = refs[8:12]
    gain, taps, decay, gate, param, offset = refs[12:18]
    normed, states = refs[18:20]
    weight, wide_decay, wide_gate = refs[20:23]
    for z_offset, piece in enumerate(pieces):
        for y_offset in range(LINE):
            weight[pl.ds(piece_of(z_offset, y_offset), 128), :] = piece[y_offset]
    wide_decay[...] = jnp.zeros(wide_decay.shape, jnp.bfloat16)
    wide_gate[...] = jnp.zeros(wide_gate.shape, jnp.bfloat16)
    for b in range(4):
        wide_decay[64 * b : 64 * b + 64, 64 * b : 64 * b + 64] = decay[b]
        wide_gate[64 * b : 64 * b + 64, 64 * b : 64 * b + 64] = gate[b]
    lean = -param[...]
    softplus = jnp.maximum(lean, 0.0) + jnp.log1p(jnp.exp(-jnp.abs(lean)))
    filters = taps[...].astype(jnp.float32)

    def sequence(s, carry):
        rows = pl.ds(pl.multiple_of(s * SEQ_LEN, SEQ_LEN), SEQ_LEN)
        norm_into(blocks, gain, rows, normed)
        values = jnp.dot(normed[rows, :], weight[...], preferred_element_type=jnp.float32)
        values = values.astype(jnp.bfloat16).astype(jnp.float32)
        total = filters[3:4] * values
        for steps in (1, 2, 3):
            total = total + filters[3 - steps : 4 - steps] * earlier(values, steps, 0.0)
        conved = total.astype(jnp.bfloat16)
        recur = jax.nn.sigmoid(
            jnp.dot(conved, wide_decay[...], preferred_element_type=jnp.float32)
        )
        inputs = jax.nn.sigmoid(
            jnp.dot(conved, wide_gate[...], preferred_element_type=jnp.float32)
        )
        log_decay = -DECAY_MULTIPLIER * recur * softplus + offset[rows, :]
        a = jnp.exp(log_decay)
        lost = -jnp.tanh(log_decay) * (a * a + 1.0)
        b = jnp.sqrt(lost) * inputs * conved.astype(jnp.float32)
        steps = 1
        while steps < SEQ_LEN:
            b = a * earlier(b, steps, 0.0) + b
            a = a * earlier(a, steps, 1.0)
            steps *= 2
        states[rows, :] = b
        return carry

    lax.fori_loop(0, 4, sequence, 0)


def project_out(left, weight, mine, theirs, rows):
    for d in range(LINE):
        for core, out in ((1, theirs), (0, mine)):
            column = column_of(d, core)
            product = jnp.dot(
                left, weight[:, pl.ds(column, 256)], preferred_element_type=jnp.float32
            )
            out[d, rows, :] = product.astype(jnp.bfloat16)


def mixer_body(*refs):
    normed, states = refs[0:2]
    pieces = refs[2:6]
    mine, theirs, gate_weight, out_weight = refs[6:10]
    for y_offset, piece in enumerate(pieces):
        for z_offset in range(LINE):
            at = piece_of(z_offset, y_offset)
            gate_weight[pl.ds(at, 128), :] = piece[z_offset, :, 0:256]
            out_weight[0:128, pl.ds(at, 128)] = piece[z_offset, :, 256:384]
            out_weight[128:256, pl.ds(at, 128)] = piece[z_offset, :, 384:512]

    def sequence(s, carry):
        rows = pl.ds(pl.multiple_of(s * SEQ_LEN, SEQ_LEN), SEQ_LEN)
        gates = jnp.dot(normed[rows, :], gate_weight[...], preferred_element_type=jnp.float32)
        gates = gates.astype(jnp.bfloat16).astype(jnp.float32)
        gelu = 0.5 * gates * (1.0 + lax.erf(gates * (0.5**0.5)))
        mixed = (states[rows, :] * gelu).astype(jnp.bfloat16)
        project_out(mixed, out_weight, mine, theirs, rows)
        return carry

    lax.fori_loop(0, 4, sequence, 0)


def pair_body(mine, theirs, *sums):
    for d, out in enumerate(sums):
        both = mine[d].astype(jnp.float32) + theirs[d].astype(jnp.float32)
        out[...] = both.astype(jnp.bfloat16)


def total_body(base, *refs):
    total = base[...].astype(jnp.float32)
    for part in refs[:-1]:
        total = total + part[...].astype(jnp.float32)
    refs[-1][...] = total.astype(jnp.bfloat16)


def feed_body(*refs):
    blocks = refs[0:8]
    ups = refs[8:12]
    downs = refs[12:16]
    gain = refs[16]
    mine, theirs, normed, up_weight, down_weight = refs[17:22]
    for other in range(LINE):
        for slot in range(LINE):
            up_weight[pl.ds(piece_of(other, slot), 128), :] = ups[other][slot]
            down_weight[:, pl.ds(piece_of(slot, other), 128)] = downs[other][slot]

    def sequence(s, carry):
        rows = pl.ds(pl.multiple_of(s * SEQ_LEN, SEQ_LEN), SEQ_LEN)
        norm_into(blocks, gain, rows, normed)
        raised = jnp.dot(normed[rows, :], up_weight[...], preferred_element_type=jnp.float32)
        activity = jnp.square(jnp.maximum(raised, 0.0)).astype(jnp.bfloat16)
        project_out(activity, down_weight, mine, theirs, rows)
        return carry

    lax.fori_loop(0, 4, sequence, 0)


def spread_and_summed(base, mine, theirs, name):
    block = jax.ShapeDtypeStruct(base.shape, jnp.bfloat16)
    sums = vmem_call(pair_body, [block] * LINE, [], name + "_pair")(mine, swapped(theirs))
    arrived = [shifted(sums[LINE - d], "x", d) for d in (1, 3, 2)]
    return vmem_call(total_body, block, [], name + "_total")(base, sums[0], *arrived)


def shards(
    stream,
    recurrent_norm_gain,
    feedforward_norm_gain,
    recurrent_input_weight,
    output_gate_weight,
    causal_filter_weight,
    decay_gate_matrix,
    input_gate_matrix,
    channel_decay_param,
    token_decay_offset,
    recurrent_output_weight,
    up_projection_weight,
    down_projection_weight,
):
    rows, columns = stream.shape
    hidden = up_projection_weight.shape[1]
    features = recurrent_norm_gain.shape[0]
    bf16 = lambda *shape: jax.ShapeDtypeStruct(shape, jnp.bfloat16)
    f32 = lambda *shape: jax.ShapeDtypeStruct(shape, jnp.float32)

    value_y = jnp.stack(from_ring(recurrent_input_weight, "y"))
    value_pieces = from_ring(value_y, Z)
    blocks = [b for pair in from_group(stream) for b in pair]
    gate_and_out = jnp.concatenate(
        [output_gate_weight, recurrent_output_weight[:128], recurrent_output_weight[128:]], axis=1
    )
    gate_z = jnp.stack(from_ring(gate_and_out, Z))
    gate_pieces = from_ring(gate_z, "y")
    up_pieces = from_ring(jnp.stack(from_ring(up_projection_weight, "y")), Z)
    down_pieces = from_ring(jnp.stack(from_ring(down_projection_weight, Z)), "y")

    normed, states = vmem_call(
        recurrence_body,
        (bf16(rows, features), f32(rows, columns)),
        [
            pltpu.VMEM((features, columns), jnp.bfloat16),
            pltpu.VMEM((columns, columns), jnp.bfloat16),
            pltpu.VMEM((columns, columns), jnp.bfloat16),
        ],
        "recurrence",
        flops=2 * rows * features * columns,
    )(
        *blocks,
        *value_pieces,
        recurrent_norm_gain.reshape(1, features),
        causal_filter_weight,
        decay_gate_matrix,
        input_gate_matrix,
        channel_decay_param.reshape(1, columns),
        token_decay_offset,
    )
    mine, theirs = vmem_call(
        mixer_body,
        (bf16(LINE, rows, columns), bf16(LINE, rows, columns)),
        [
            pltpu.VMEM((features, columns), jnp.bfloat16),
            pltpu.VMEM((columns, features), jnp.bfloat16),
        ],
        "mixer",
        flops=4 * rows * features * columns,
    )(normed, states, *gate_pieces)
    middle = spread_and_summed(stream, mine, theirs, "mixer")
    middle_blocks = [b for pair in from_group(middle) for b in pair]
    mine, theirs = vmem_call(
        feed_body,
        (bf16(LINE, rows, columns), bf16(LINE, rows, columns)),
        [
            pltpu.VMEM((rows, features), jnp.bfloat16),
            pltpu.VMEM((features, hidden), jnp.bfloat16),
            pltpu.VMEM((hidden, features), jnp.bfloat16),
        ],
        "feed",
        flops=4 * rows * features * hidden,
    )(*middle_blocks, *up_pieces, *down_pieces, feedforward_norm_gain.reshape(1, features))
    return spread_and_summed(middle, mine, theirs, "feed")


def solution(mesh):
    split = Mesh(
        mesh.devices.reshape(mesh.shape["rep"], 4, 4, 4, 2),
        ("zh", "zl", "y", "x", "c"),
    )
    placed = (
        P(REP_FS, TP),
        P(),
        P(),
        P(FS, TP),
        P(FS, TP),
        P(None, TP),
        P(TP, None, None),
        P(TP, None, None),
        P(TP),
        P(REP_FS, TP),
        P(TP, FS),
        P(FS, TP),
        P(TP, FS),
    )
    return jax.shard_map(
        shards, mesh=split, in_specs=placed, out_specs=P(REP_FS, TP), check_vma=False
    )
```
